512 devices in a mesh: fs: 32 (over z, core), tp: 16 (over y, x).
Axes of the slice: x: 4, y: 4, z: 16, core: 2. Of those that a mesh axis runs over, the one named last changes fastest.
Arguments:
- tokens: bfloat16 [8192, 2048], P('fs', 'tp'), may hold values from -6 to 6
- norm_gain: float32 [2048], P('tp'), may hold values from 0.1 to 1.9
- gate_master: float32 [16, 3584, 2048], P(None, 'fs', 'tp'), may hold values from -0.125 to 0.125
- up_master: float32 [16, 3584, 2048], P(None, 'fs', 'tp'), may hold values from -0.125 to 0.125
- down_master: float32 [16, 3584, 2048], P(None, 'fs', 'tp'), may hold values from -0.0625 to 0.0625
- routes: int32 [8192, 2], P('fs'), may hold values from 0 to 7, all different within a row; in each aligned block of 256 rows (0 to 255, 256 to 511, ...) at most 64 rows name the same one
- route_logits: float32 [8192, 2], P('fs'), may hold values from -8 to 8
Outputs:
- gate_serve: bfloat16 [16, 3584, 2048], P('tp', 'fs')
- up_serve: bfloat16 [16, 3584, 2048], P('tp', 'fs')
- down_serve: bfloat16 [16, 3584, 2048], P('tp', 'fs')
- mixed_tokens: bfloat16 [8192, 2048], P('fs', 'tp')
The draws below stay inside these ranges and needn't reach their ends.
Inputs may be any that keep to these rules, and one draw needn't show every extreme that they name: `routes`: each row names 2 different experts; in every aligned block of 256 rows each expert is named by exactly 64 rows.
All inputs are finite; a program needn't handle non-finite values.
Results may differ from the reference program's by a relative error of at most 0.024.
Values may be sent and summed in bfloat16 or wider, within the bound.
A program may use at most 64 MiB of HBM per device.

```python
import math
import jax
import jax.numpy as jnp
import numpy as np
from jax import lax

D = 2048
FF = 7168
TOP = 2
TOK_DEV = 256
EXPERTS = 8
SLABS = 16
FF_SLAB = 3584
TOKENS = 8192
CAP = 64
N_FS = 32


def block_levels(key, extent, pieces, low, top_value):
    def one(position, shards_of):
        steps = jax.random.uniform(jax.random.fold_in(jax.random.fold_in(key, 6), position), (shards_of,), jnp.float32, low / len(pieces), top_value / len(pieces))
        return jnp.repeat(jnp.exp(steps), extent[position] // shards_of).reshape((-1,) + (1,) * (len(extent) - position - 1))

    factor_of = one(*pieces[0])
    for cut in pieces[1:]:
        factor_of = factor_of * one(*cut)
    return factor_of


def assign_block(own_key, own, number, rows, number_of, top, bound, lean):
    order = jax.random.permutation(own_key, number_of)
    crowded, common = portions_of(number_of, rows * top, bound, lean, True), portions_of(number_of, rows * top, bound, lean, False)
    places = jnp.arange(number_of)

    def named(sizes, offset_by):
        used = int((sizes > 0).sum())
        fixed = max(1, used // 4)
        shifted = fixed + (places - fixed + offset_by * (used - fixed)) % max(1, number_of - fixed)
        return jnp.zeros((number_of,), jnp.int32).at[order[jnp.where(places < fixed, places, shifted)]].set(jnp.asarray(sizes, jnp.int32))

    sizes = jnp.where(number % 4 == 0, named(crowded, number // 4), named(common, number - number // 4 - 1))
    mixed = jax.random.permutation(jax.random.fold_in(own, 3), number_of)
    giver, sink = mixed[0:number_of // 2 * 2:2], mixed[1:number_of // 2 * 2:2]
    margin = jnp.minimum(sizes[giver] - 1, bound - sizes[sink]) // 2
    margin = jnp.where((giver == order[0]) | (sink == order[0]) | (sizes[sink] == 0), 0, jnp.maximum(margin, 0))
    shifted = jax.random.randint(jax.random.fold_in(own, 4), (number_of // 2,), 0, 1 << 20) % (margin + 1)
    sizes = sizes.at[giver].add(-shifted).at[sink].add(shifted)
    items = jnp.searchsorted(jnp.cumsum(sizes), jnp.arange(rows * top), side="right").astype(jnp.int32)
    grid = items.reshape(top, rows).T
    grid = grid[jax.random.permutation(jax.random.fold_in(own, 1), rows)]
    offset_by = jax.random.randint(jax.random.fold_in(own, 2), (rows, 1), 0, top)
    return jnp.take_along_axis(grid, (jnp.arange(top)[None, :] + offset_by) % top, axis=1)


def portions_of(number_of, total, limit, slope, full):
    weights = [(1 << 20) // math.isqrt(standing ** slope) + 1 for standing in range(1, number_of + 1)]
    largest = limit if full else min(limit, max(-(-total // number_of), total * weights[0] // sum(weights)))
    least = 1 if total - largest >= number_of - 1 else 0
    counts, spare = [largest] + [least] * (number_of - 1), total - largest - least * (number_of - 1)
    while spare > 0:
        candidates = [i for i in range(1, number_of) if counts[i] < largest] or [i for i in range(1, number_of) if counts[i] < limit]
        pool, left = sum([weights[i] for i in candidates]), spare
        for i in candidates:
            addition = min(limit - counts[i], max(1, left * weights[i] // pool), spare)
            counts[i] = counts[i] + addition
            spare = spare - addition
    return np.array(counts)


def normal_values(key, shape, width, limit, split=(), kind=jnp.bfloat16):
    drawn = width * jax.random.normal(key, shape, jnp.float32)
    if split:
        drawn = drawn * block_levels(key, shape, split, -0.22, 0.18)
    return jnp.clip(drawn, -limit, limit).astype(kind)


def setup_inputs(seed: int = 0) -> dict:
    seeds = jax.random.split(jax.random.key(seed), 8)
    tokens = normal_values(seeds[0], (TOKENS, D), 1.0, 6.0, ((0, 32), (1, 16)))
    norm_gain = jnp.clip(1.0 + 0.18 * jax.random.normal(seeds[1], (D,), jnp.float32), 0.1, 1.9)
    gate_master = normal_values(seeds[2], (SLABS, FF_SLAB, D), D ** -0.5, 0.125, ((1, 32), (2, 16)), jnp.float32)
    up_master = normal_values(seeds[3], (SLABS, FF_SLAB, D), D ** -0.5, 0.125, ((1, 32), (2, 16)), jnp.float32)
    down_master = normal_values(seeds[4], (SLABS, FF_SLAB, D), FF ** -0.5, 0.0625, ((1, 32), (2, 16)), jnp.float32)
    routes_keys = jax.random.split(jax.random.fold_in(seeds[5], 1), TOKENS // TOK_DEV)
    routes_turns = jax.random.permutation(jax.random.fold_in(seeds[5], 3), TOKENS // TOK_DEV)
    routes = jax.vmap(lambda own, number: assign_block(jax.random.fold_in(seeds[5], 2), own, number, TOK_DEV, EXPERTS, TOP, CAP, 0))(routes_keys, routes_turns).reshape((TOKENS, TOP))
    route_logits = normal_values(seeds[6], (TOKENS, TOP), 2.0, 8.0, ((0, 32),), jnp.float32)
    return dict(tokens=tokens, norm_gain=norm_gain, gate_master=gate_master, up_master=up_master, down_master=down_master, routes=routes, route_logits=route_logits)


epsilon = 1e-05

def reference(tokens, norm_gain, gate_master, up_master, down_master, routes, route_logits):
    gain_row = norm_gain[None, None, :]
    gate_serve = (gate_master * gain_row).astype(jnp.bfloat16)
    up_serve = (up_master * gain_row).astype(jnp.bfloat16)
    down_serve = down_master.astype(jnp.bfloat16)
    widened = tokens.astype(jnp.float32)
    row_scale = lax.rsqrt(lax.optimization_barrier(jnp.mean(widened * widened, axis=-1, keepdims=True)) + epsilon)
    normed = (widened * row_scale).astype(jnp.bfloat16)
    first_prob = jax.nn.sigmoid(route_logits[:, 0] - route_logits[:, 1])
    choice_prob = jnp.stack([first_prob, 1.0 - first_prob], axis=1)
    row_total = N_FS * CAP
    block_rows = FF_SLAB // N_FS

    def one_expert(expert_id):
        matches = routes == expert_id
        is_member = jnp.any(matches, axis=1)
        weight = lax.optimization_barrier(jnp.sum(jnp.where(matches, choice_prob, 0.0), axis=1))
        row_index = jnp.nonzero(is_member, size=row_total)[0].astype(jnp.int32)
        picked = normed[row_index]
        block_parts = jnp.zeros((N_FS, row_total, D), jnp.float32)
        for half_index in range(2):
            slab_id = 2 * expert_id + half_index
            gate_slab = lax.dynamic_index_in_dim(gate_serve, slab_id, 0, keepdims=False)
            up_slab = lax.dynamic_index_in_dim(up_serve, slab_id, 0, keepdims=False)
            down_slab = lax.dynamic_index_in_dim(down_serve, slab_id, 0, keepdims=False)
            gate_pre = jnp.dot(picked, gate_slab.T, preferred_element_type=jnp.float32)
            up_pre = jnp.dot(picked, up_slab.T, preferred_element_type=jnp.float32)
            hidden = (jax.nn.silu(gate_pre) * up_pre).astype(jnp.bfloat16)
            block_parts = block_parts + jnp.einsum('rfk,fkd->frd', hidden.reshape(row_total, N_FS, block_rows).astype(jnp.float32), down_slab.reshape(N_FS, block_rows, D).astype(jnp.float32))
        rounded = lax.optimization_barrier(block_parts.astype(jnp.bfloat16))
        expert_out = lax.optimization_barrier(jnp.sum(rounded.astype(jnp.float32), axis=0)).astype(jnp.bfloat16)
        return (row_index, weight[row_index][:, None] * expert_out.astype(jnp.float32))
    expert_ids = jnp.arange(EXPERTS, dtype=jnp.int32)
    all_index, all_terms = lax.map(one_expert, expert_ids)
    mixed = jnp.zeros((TOKENS, D), jnp.float32).at[all_index.reshape(-1)].add(all_terms.reshape(-1, D))
    return (gate_serve, up_serve, down_serve, mixed.astype(jnp.bfloat16))
```

```python
import functools

import jax
import jax.numpy as jnp
from jax import lax
from jax.experimental import pallas as pl
from jax.experimental.pallas import tpu as pltpu
from jax.sharding import PartitionSpec as P

EPS = 1e-05
NX = 4
NT = 16
LANES = 128
MESH = pl.DeviceIdType.MESH
GROUPS = ((0, 2), (2, 1))
NG = len(GROUPS)


def kernel(
    nz,
    picked,
    wsrc,
    gate_out,
    up_out,
    down_out,
    ret,
    rows,
    ybuf,
    wbuf,
    xn,
    hid,
    part,
    rs_in,
    rs_out,
    eo,
    tok_s,
    tok_r,
    ag_s,
    ag_r,
    y_s,
    y_r,
    x_s,
    x_r,
    d_s,
    d_r,
    rs_s,
    rs_r,
    fin_s,
    fin_r,
    out_s,
):
    rb = rows.shape[1]
    width = rows.shape[2]
    fb = wsrc.shape[1] // NT
    pair = 2 * fb
    half = nz // 2
    cw = width // 2
    fs = lax.axis_index("fs")
    tp = lax.axis_index("tp")
    z, core = fs // 2, lax.rem(fs, 2)
    y, x = tp // NX, lax.rem(tp, NX)
    px, h = x // 2, lax.rem(x, 2)
    mate = {"tp": tp + 1 - 2 * h}
    cross = {"tp": y * NX + (NX - 1) - x}
    other_core = {"fs": fs + 1 - 2 * core}
    z_up = {"fs": lax.rem(z + 1, nz) * 2 + core}
    z_down = {"fs": lax.rem(z + nz - 1, nz) * 2 + core}
    z_dev = (z_up, z_down)
    pending = []

    def send(src, dst, s, r, dev):
        c = pltpu.make_async_remote_copy(
            src_ref=src, dst_ref=dst, send_sem=s, recv_sem=r, device_id=dev, device_id_type=MESH
        )
        c.start()
        pending.append(c)
        return c

    barrier = pltpu.get_barrier_semaphore()
    for k in range(1, NT):
        pl.semaphore_signal(
            barrier, inc=1, device_id={"tp": lax.rem(tp + k, NT)}, device_id_type=MESH
        )
    for dev in (other_core, z_up, z_down):
        pl.semaphore_signal(barrier, inc=1, device_id=dev, device_id_type=MESH)
    pl.semaphore_wait(barrier, NT - 1 + 3)

    lanes = lambda t: pl.ds(pl.multiple_of(t * LANES, LANES), LANES)
    frow = lambda i, n: pl.ds(pl.multiple_of(i * fb, fb), n * fb)
    my_rows = frow(2 * core, 2)

    tok = [None]
    for k in range(1, NT):
        t = lax.rem(tp + k, NT)
        tok.append(
            send(picked.at[t], rows.at[z, :, lanes(tp)], tok_s.at[k], tok_r.at[k], {"tp": t})
        )
    y_c = []
    for k in range(1, NX):
        ty = lax.rem(y + k, NX)
        dev = {"tp": ty * NX + x}
        per = []
        for g, (a, n) in enumerate(GROUPS):
            mine = send(
                wsrc.at[pl.ds(a, n), frow(ty * NX + 2 * px, 2), :],
                wbuf.at[pl.ds(a, n), my_rows, lanes(tp)],
                y_s.at[k - 1, g, 0],
                y_r.at[k - 1, g, 0],
                dev,
            )
            theirs = send(
                wsrc.at[pl.ds(a, n), frow(ty * NX + 2 - 2 * px, 2), :],
                ybuf.at[k - 1, pl.ds(a, n)],
                y_s.at[k - 1, g, 1],
                y_r.at[k - 1, g, 1],
                dev,
            )
            per.append((mine, theirs))
        y_c.append(per)

    x_c = {}

    def x_send(q):
        col = lax.rem(y + NX - q, NX) * NX + x
        for g, (a, n) in enumerate(GROUPS):
            if q:
                y_c[q - 1][g][0].wait_recv()
                y_c[q - 1][g][1].wait_recv()
                own = wbuf.at[pl.ds(a, n), my_rows, lanes(col)]
                oth = ybuf.at[q - 1, pl.ds(a, n)]
            else:
                own = wsrc.at[pl.ds(a, n), frow(y * NX + 2 * px, 2), :]
                oth = wsrc.at[pl.ds(a, n), frow(y * NX + 2 - 2 * px, 2), :]
            dst = wbuf.at[pl.ds(a, n), my_rows, lanes(col)]
            x_c[q, g, 1] = send(oth, dst, x_s.at[q, g, 1], x_r.at[q, g, 1], cross)
            x_c[q, g, 0] = send(own, dst, x_s.at[q, g, 0], x_r.at[q, g, 0], mate)

    def x_forward(q):
        col = lax.rem(y + NX - q, NX) * NX + (NX - 1) - x
        for g, (a, n) in enumerate(GROUPS):
            x_c[q, g, 1].wait_recv()
            ref = wbuf.at[pl.ds(a, n), my_rows, lanes(col)]
            x_c[q, g, 2] = send(ref, ref, x_s.at[q, g, 2], x_r.at[q, g, 2], mate)

    d_c = {}

    def core_send(q):
        cols = pl.ds(
            pl.multiple_of(lax.rem(y + NX - q, NX) * NX * LANES, NX * LANES), NX * LANES
        )
        for g, (a, n) in enumerate(GROUPS):
            x_c[q, g, 0].wait_recv()
            x_c[q, g, 2].wait_recv()
            ref = wbuf.at[pl.ds(a, n), my_rows, cols]
            d_c[q, g] = send(ref, ref, d_s.at[q, g], d_r.at[q, g], other_core)

    x_send(0)
    rows[z, :, lanes(tp)] = picked[tp]
    for a in range(3):
        wbuf[a, my_rows, lanes(tp)] = wsrc[a, frow(y * NX + 2 * px, 2), :]

    ag_c = {}

    def ag_chunks(s, d):
        return (0, 1) if s < half - 1 else (d,)

    def ag_send(s, d, c):
        b = lax.rem(z + (nz - s if d == 0 else s), nz)
        ref = rows.at[b, :, pl.ds(c * cw, cw)]
        ag_c[s, d, c] = send(ref, ref, ag_s.at[d, s, c], ag_r.at[d, s, c], z_dev[d])

    def ag_step(s):
        for c in (0, 1):
            for d in (0, 1):
                if s and c in ag_chunks(s - 1, d):
                    ag_c[s - 1, d, c].wait_recv()
                if s < half and c in ag_chunks(s, d):
                    ag_send(s, d, c)

    for k in range(1, NT):
        tok[k].wait_recv()
    ag_step(0)
    x_forward(0)
    ag_step(1)
    x_send(1)
    ag_step(2)
    x_send(3)
    x_forward(1)
    core_send(0)
    ag_step(3)
    x_forward(3)
    ag_step(4)
    core_send(1)
    ag_step(5)
    x_send(2)
    ag_step(6)
    core_send(3)
    x_forward(2)
    for s in range(7, half + 1):
        ag_step(s)

    @pl.loop(0, nz)
    def _(b):
        wide = rows[b].astype(jnp.float32)
        scale = lax.rsqrt(jnp.mean(wide * wide, axis=-1, keepdims=True) + EPS)
        xn[pl.ds(pl.multiple_of(b * rb, rb), rb), :] = (wide * scale).astype(jnp.bfloat16)

    core_send(2)
    outs = []
    for a, out in enumerate((gate_out, up_out, down_out)):
        c = pltpu.make_async_copy(wbuf.at[a, frow(2 * core + h, 1), :], out, out_s.at[a])
        c.start()
        outs.append(c)
    for q in range(NX):
        for g in range(NG):
            d_c[q, g].wait_recv()

    nt = (((1,), (1,)), ((), ()))

    @pl.loop(0, 2)
    def _(c):
        f = pl.ds(pl.multiple_of(c * pair, pair), pair)
        gate = lax.dot_general(xn[...], wbuf[0, f, :], nt, preferred_element_type=jnp.float32)
        up = lax.dot_general(xn[...], wbuf[1, f, :], nt, preferred_element_type=jnp.float32)
        hid[c] = (jax.nn.silu(gate) * up).astype(jnp.bfloat16)

    @pl.loop(0, width // 512)
    def _(i):
        cols = pl.ds(pl.multiple_of(i * 512, 512), 512)
        part[:, cols] = jnp.dot(
            hid[0], wbuf[2, pl.ds(0, pair), cols], preferred_element_type=jnp.float32
        ) + jnp.dot(hid[1], wbuf[2, pl.ds(pair, pair), cols], preferred_element_type=jnp.float32)

    rs_c = {}

    def term(b, c):
        return part[pl.ds(pl.multiple_of(b * rb, rb), rb), pl.ds(c * cw, cw)]

    for s in range(half):
        for c in (0, 1):
            for d in (0, 1):
                if s == 0 and c != d:
                    continue
                b = lax.rem(z + (half - s if d == 0 else half + s), nz)
                acc = term(b, c)
                if (s - 1, d, c) in rs_c:
                    rs_c[s - 1, d, c].wait_recv()
                    acc = acc + rs_in[d, s - 1, c].astype(jnp.float32)
                rs_out[d, s, c] = acc.astype(jnp.bfloat16)
                rs_c[s, d, c] = send(
                    rs_out.at[d, s, c],
                    rs_in.at[d, s, c],
                    rs_s.at[d, s, c],
                    rs_r.at[d, s, c],
                    z_dev[d],
                )
    for c in (0, 1):
        acc = term(z, c)
        for d in (0, 1):
            rs_c[half - 1, d, c].wait_recv()
            acc = acc + rs_in[d, half - 1, c].astype(jnp.float32)
        eo[:, pl.ds(c * cw, cw)] = acc.astype(jnp.bfloat16)

    fin = []
    mine = pl.ds(pl.multiple_of(tp * rb, rb), rb)
    for k in range(1, NT):
        t = lax.rem(tp + k, NT)
        fin.append(
            send(eo.at[:, lanes(t)], ret.at[mine, :], fin_s.at[k], fin_r.at[k], {"tp": t})
        )
    ret[mine, :] = eo[:, lanes(tp)]
    for c in fin:
        c.wait_recv()
    for c in outs:
        c.wait()
    for c in pending:
        c.wait_send()


def exchange(picked, wsrc, nz):
    rb, width, fb = picked.shape[1], NT * LANES, wsrc.shape[1] // NT
    half, cw = nz // 2, width // 2
    bf16, f32 = jnp.bfloat16, jnp.float32
    dma = pltpu.SemaphoreType.DMA
    vmem = pl.BlockSpec(memory_space=pltpu.VMEM)
    hbm = pl.BlockSpec(memory_space=pl.ANY)
    return pl.pallas_call(
        functools.partial(kernel, nz),
        name="exchange",
        out_shape=[jax.ShapeDtypeStruct((1, fb, width)[1:], bf16)] * 3
        + [jax.ShapeDtypeStruct((NT * rb, LANES), bf16)],
        in_specs=[vmem, vmem],
        out_specs=[hbm, hbm, hbm, vmem],
        scratch_shapes=[
            pltpu.VMEM((nz, rb, width), bf16),
            pltpu.VMEM((NX - 1, 3, 2 * fb, LANES), bf16),
            pltpu.VMEM((3, 4 * fb, width), bf16),
            pltpu.VMEM((nz * rb, width), bf16),
            pltpu.VMEM((2, nz * rb, 2 * fb), bf16),
            pltpu.VMEM((nz * rb, width), f32),
            pltpu.VMEM((2, half, 2, rb, cw), bf16),
            pltpu.VMEM((2, half, 2, rb, cw), bf16),
            pltpu.VMEM((rb, width), bf16),
            dma((NT,)),
            dma((NT,)),
            dma((2, half, 2)),
            dma((2, half, 2)),
            dma((NX - 1, NG, 2)),
            dma((NX - 1, NG, 2)),
            dma((NX, NG, 3)),
            dma((NX, NG, 3)),
            dma((NX, NG)),
            dma((NX, NG)),
            dma((2, half, 2)),
            dma((2, half, 2)),
            dma((NT,)),
            dma((NT,)),
            dma((3,)),
        ],
        compiler_params=pltpu.CompilerParams(collective_id=0, has_side_effects=True),
    )(picked, wsrc)


def local(tokens, norm_gain, gate_master, up_master, down_master, routes, route_logits):
    tok_rows = tokens.shape[0]
    experts = NT // 2
    capacity = tok_rows * 2 // experts
    fb = gate_master.shape[1]
    gain_row = norm_gain[None, None, :]
    wsrc = jnp.stack(
        [
            (gate_master * gain_row).astype(jnp.bfloat16),
            (up_master * gain_row).astype(jnp.bfloat16),
            down_master.astype(jnp.bfloat16),
        ]
    ).reshape(3, NT * fb, LANES)
    first_prob = jax.nn.sigmoid(route_logits[:, 0] - route_logits[:, 1])
    ids = jnp.arange(experts, dtype=jnp.int32)
    match = [routes[:, k][:, None] == ids[None, :] for k in (0, 1)]
    chosen = (match[0] | match[1]).astype(jnp.bfloat16)
    row_ids = jnp.arange(tok_rows, dtype=jnp.int32)
    before = (row_ids[None, :] < row_ids[:, None]).astype(jnp.bfloat16)
    position = jnp.dot(before, chosen, preferred_element_type=jnp.float32).astype(jnp.int32)
    slot_of = ids[None, :] * capacity + position
    slots = jnp.arange(experts * capacity, dtype=jnp.int32)
    hot = []
    for k in (0, 1):
        slot = jnp.sum(jnp.where(match[k], slot_of, 0), axis=1)
        hot.append((slot[:, None] == slots[None, :]).astype(jnp.bfloat16))
    both = hot[0] + hot[1]
    picked = lax.dot_general(
        both, tokens, (((0,), (0,)), ((), ())), preferred_element_type=jnp.float32
    ).astype(jnp.bfloat16)
    nz = lax.axis_size("fs") // 2
    gate_serve, up_serve, down_serve, ret = exchange(
        picked.reshape(NT, capacity // 2, LANES), wsrc, nz
    )
    sent = [jnp.dot(m, ret, preferred_element_type=jnp.float32) for m in hot]
    mixed = first_prob[:, None] * sent[0] + (1.0 - first_prob)[:, None] * sent[1]
    return (gate_serve[None], up_serve[None], down_serve[None], mixed.astype(jnp.bfloat16))


def solution(mesh):
    weights = P(None, "fs", "tp")
    served = P("tp", "fs", None)
    return jax.shard_map(
        local,
        mesh=mesh,
        in_specs=(P("fs", "tp"), P("tp"), weights, weights, weights, P("fs"), P("fs")),
        out_specs=(served, served, served, P("fs", "tp")),
        check_vma=False,
    )
```

```python
import contextlib
import functools

import jax
import jax.numpy as jnp
from jax import lax
from jax.experimental import pallas as pl
from jax.experimental.pallas import tpu as pltpu
from jax.sharding import PartitionSpec as P

EPS = 1e-05
NX = 4
NT = 16
LANES = 128
QC = NX * LANES
MESH = pl.DeviceIdType.MESH
GROUPS = ((0, 2), (2, 1))
NG = len(GROUPS)
QORD = (0, 1, 3, 2)
SPLIT = ((0, 1), (3, 2))
SCOPED = False
ORDER = (
    "T0 T1 T3 T2 F0a X0b A1 X1a X3a Ra A2 F1a F3a F0b A3 X2a C0a C1a A4 F2a C3a X1b X3b Rb A5 "
    "F1b F3b C0b X2b A6 C2a F2b C1b A7 C3b H A8 C2b"
).split()


def scope(name):
    return jax.named_scope(name) if SCOPED else contextlib.nullcontext()


def kernel(
    nz,
    tokens_h,
    gain_h,
    gate_h,
    up_h,
    down_h,
    routes_h,
    logits_h,
    gate_out,
    up_out,
    down_out,
    mixed_out,
    tokens,
    gain,
    masters,
    routes,
    logits,
    wsrc,
    picked,
    cols8,
    rows,
    scales,
    ybuf,
    relay,
    wbuf,
    hid,
    part,
    rs_in,
    rs_out,
    eo,
    ret,
    in_s,
    tok_s,
    tok_r,
    ag_s,
    ag_r,
    y_s,
    y_r,
    w_s,
    w_r,
    x_s,
    x_r,
    d_s,
    d_r,
    rs_s,
    rs_r,
    fin_s,
    fin_r,
    out_s,
):
    tr = tokens.shape[0]
    width = rows.shape[1]
    rb = rows.shape[0] // nz
    fb = wsrc.shape[1] // NT
    pair = 2 * fb
    half = nz // 2
    f32, bf16 = jnp.float32, jnp.bfloat16
    fs = lax.axis_index("fs")
    tp = lax.axis_index("tp")
    z, core = fs // 2, lax.rem(fs, 2)
    y, x = tp // NX, lax.rem(tp, NX)
    px, h = x // 2, lax.rem(x, 2)
    mate = {"tp": tp + 1 - 2 * h}
    cross = {"tp": y * NX + (NX - 1) - x}
    other_core = {"fs": fs + 1 - 2 * core}
    z_up = {"fs": lax.rem(z + 1, nz) * 2 + core}
    z_down = {"fs": lax.rem(z + nz - 1, nz) * 2 + core}
    z_dev = (z_up, z_down)
    pending = []

    def send(src, dst, s, r, dev):
        c = pltpu.make_async_remote_copy(
            src_ref=src, dst_ref=dst, send_sem=s, recv_sem=r, device_id=dev, device_id_type=MESH
        )
        c.start()
        pending.append(c)
        return c

    def plane(dy, dx):
        return lax.rem(y + dy, NX) * NX + lax.rem(x + dx, NX)

    barrier = pltpu.get_barrier_semaphore()
    for k in range(1, NT):
        pl.semaphore_signal(
            barrier, inc=1, device_id={"tp": lax.rem(tp + k, NT)}, device_id_type=MESH
        )
    for dev in (other_core, z_up, z_down):
        pl.semaphore_signal(barrier, inc=1, device_id=dev, device_id_type=MESH)

    loads = []
    for i, (src, dst) in enumerate(
        (
            (routes_h, routes),
            (logits_h, logits),
            (tokens_h, tokens),
            (gain_h, gain),
            (gate_h, masters.at[0]),
            (up_h, masters.at[1]),
            (down_h, masters.at[2]),
        )
    ):
        c = pltpu.make_async_copy(src, dst, in_s.at[i])
        c.start()
        loads.append(c)

    lanes = lambda t: pl.ds(pl.multiple_of(t * LANES, LANES), LANES)
    frow = lambda i, n: pl.ds(pl.multiple_of(i * fb, fb), n * fb)
    chunk = lambda q: pl.ds(pl.multiple_of(lax.rem(y + NX - q, NX) * QC, QC), QC)
    src_tp = lambda q, xx: lax.rem(y + NX - q, NX) * NX + xx
    my_rows = frow(2 * core, 2)

    with scope("prep"):
        for c in loads[:4]:
            c.wait()
        e = lax.broadcasted_iota(jnp.int32, (NT // 2, tr), 0)
        m0 = e == routes[0:1, :]
        m1 = e == routes[1:2, :]
        chosen = jnp.where(m0 | m1, 1.0, 0.0).astype(bf16)
        earlier = lax.broadcasted_iota(jnp.int32, (tr, tr), 0) < lax.broadcasted_iota(
            jnp.int32, (tr, tr), 1
        )
        pos = jnp.dot(
            chosen, jnp.where(earlier, 1.0, 0.0).astype(bf16), preferred_element_type=f32
        )
        slot = pos + (2 * rb) * e.astype(f32)
        s0 = jnp.sum(jnp.where(m0, slot, 0.0), axis=0, keepdims=True)
        s1 = jnp.sum(jnp.where(m1, slot, 0.0), axis=0, keepdims=True)
        ids = lax.broadcasted_iota(jnp.int32, (NT * rb, tr), 0).astype(f32)
        hot = jnp.where((ids == s0) | (ids == s1), 1.0, 0.0).astype(bf16)
        picked[...] = jnp.dot(hot, tokens[...], preferred_element_type=f32).astype(bf16)
        p0 = jax.nn.sigmoid(logits[0:1, :] - logits[1:2, :])
        table = jnp.concatenate([s0, s1, p0, 1.0 - p0, jnp.zeros((4, tr), f32)], axis=0)
        cols8[...] = table.T
        for a in range(3):
            loads[4 + a].wait()
            if a < 2:
                wsrc[a] = (masters[a] * gain[...]).astype(bf16)
            else:
                wsrc[a] = masters[a].astype(bf16)
    with scope("barrier"):
        pl.semaphore_wait(barrier, NT - 1 + 3)

    prow = lambda t: pl.ds(pl.multiple_of(t * rb, rb), rb)
    tok = {}
    for dy in QORD:
        for dx in range(NX):
            if dy or dx:
                t = plane(dy, dx)
                tok[dy, dx] = send(
                    picked.at[prow(t), :],
                    rows.at[pl.ds(0, rb), lanes(tp)],
                    tok_s.at[dy, dx],
                    tok_r.at[dy, dx],
                    {"tp": t},
                )

    y_c, w_c = {}, {}

    def y_send(g):
        a, n = GROUPS[g]
        ks = pl.ds(a, n)
        for k in (1, 3):
            ty = lax.rem(y + k, NX)
            dev = {"tp": ty * NX + x}
            y_c[k, g, 0] = send(
                wsrc.at[ks, frow(ty * NX + 2 * px, 2), :],
                wbuf.at[ks, my_rows, lanes(tp)],
                y_s.at[k - 1, g, 0],
                y_r.at[k - 1, g, 0],
                dev,
            )
            y_c[k, g, 1] = send(
                wsrc.at[ks, frow(ty * NX + 2 - 2 * px, 2), :],
                ybuf.at[k - 1, ks],
                y_s.at[k - 1, g, 1],
                y_r.at[k - 1, g, 1],
                dev,
            )
        ty = lax.rem(y + 2, NX)
        for i, (first, via) in enumerate(((2 * px, 1), (2 - 2 * px, 3))):
            w_c[g, i] = send(
                wsrc.at[ks, frow(ty * NX + first, 2), :],
                relay.at[i, ks],
                w_s.at[g, i],
                w_r.at[g, i],
                {"tp": lax.rem(y + via, NX) * NX + x},
            )

    def y_relay(g):
        a, n = GROUPS[g]
        ks = pl.ds(a, n)
        for i, via in enumerate((1, 3)):
            w_c[g, i].wait_recv()
            dst = wbuf.at[ks, my_rows, lanes(src_tp(via, x))] if i == 0 else ybuf.at[1, ks]
            y_c[2, g, i] = send(
                relay.at[i, ks],
                dst,
                y_s.at[1, g, i],
                y_r.at[1, g, i],
                {"tp": lax.rem(y + via, NX) * NX + x},
            )

    x_c = {}

    def x_send(q, g):
        a, n = GROUPS[g]
        ks = pl.ds(a, n)
        dst = wbuf.at[ks, my_rows, lanes(src_tp(q, x))]
        if q:
            y_c[q, g, 1].wait_recv()
            oth = ybuf.at[q - 1, ks]
        else:
            oth = wsrc.at[ks, frow(y * NX + 2 - 2 * px, 2), :]
        x_c[q, g, 1] = send(oth, dst, x_s.at[q, g, 1], x_r.at[q, g, 1], cross)
        if q:
            y_c[q, g, 0].wait_recv()
            own = dst
        else:
            own = wsrc.at[ks, frow(y * NX + 2 * px, 2), :]
        x_c[q, g, 0] = send(own, dst, x_s.at[q, g, 0], x_r.at[q, g, 0], mate)

    def x_forward(q, g):
        a, n = GROUPS[g]
        x_c[q, g, 1].wait_recv()
        ref = wbuf.at[pl.ds(a, n), my_rows, lanes(src_tp(q, (NX - 1) - x))]
        x_c[q, g, 2] = send(ref, ref, x_s.at[q, g, 2], x_r.at[q, g, 2], mate)

    d_c = {}

    def core_send(q, g):
        a, n = GROUPS[g]
        x_c[q, g, 0].wait_recv()
        x_c[q, g, 2].wait_recv()
        ref = wbuf.at[pl.ds(a, n), my_rows, chunk(q)]
        d_c[q, g] = send(ref, ref, d_s.at[q, g], d_r.at[q, g], other_core)

    down_of = lambda j: 2 * j - 1 if j else 0
    up_of = lambda j: nz - 1 if j == half else 2 * j
    at = lambda p: pl.ds(p * rb, rb)
    ag_c = {}

    def ag_has(s, d, q):
        return s < half - 1 or q in SPLIT[d]

    def ag_send(s, d, q):
        of = (down_of, up_of)[d]
        ag_c[s, d, q] = send(
            rows.at[at(of(s)), chunk(q)],
            rows.at[at(of(s + 1)), chunk(q)],
            ag_s.at[d, s, q],
            ag_r.at[d, s, q],
            z_dev[d],
        )

    def scale_of(p, n):
        r = pl.ds(p * rb, n * rb)
        wide = rows[r, :].astype(f32)
        scales[r, :] = lax.rsqrt(jnp.mean(wide * wide, axis=-1, keepdims=True) + EPS)

    def ag_first(q):
        for dx in range(NX):
            if q or dx:
                tok[q, dx].wait_recv()
        for d in (0, 1):
            ag_send(0, d, q)

    def ag_step(s):
        for q in QORD:
            for d in (0, 1):
                if ag_has(s - 1, d, q):
                    ag_c[s - 1, d, q].wait_recv()
                if s < half and ag_has(s, d, q):
                    ag_send(s, d, q)
        if s == half:
            scale_of(nz - 1, 1)
        else:
            scale_of(down_of(s), 2)

    nt = (((1,), (1,)), ((), ()))

    def hidden(p, n):
        r = pl.ds(p * rb, n * rb)

        @pl.loop(0, 2)
        def _(c):
            f = pl.ds(pl.multiple_of(c * pair, pair), pair)
            s = scales[r, :]
            xr = rows[r, :]
            gate = s * lax.dot_general(xr, wbuf[0, f, :], nt, preferred_element_type=f32)
            up = s * lax.dot_general(xr, wbuf[1, f, :], nt, preferred_element_type=f32)
            hid[c, r, :] = (jax.nn.silu(gate) * up).astype(bf16)

    def project(p, n, q):
        r = pl.ds(p * rb, n * rb)
        part[r, chunk(q)] = jnp.dot(
            hid[0, r, :], wbuf[2, pl.ds(0, pair), chunk(q)], preferred_element_type=f32
        ) + jnp.dot(hid[1, r, :], wbuf[2, pl.ds(pair, pair), chunk(q)], preferred_element_type=f32)

    def gate_up_here():
        for q in QORD:
            d_c[q, 0].wait_recv()

    y_send(0)
    x_send(0, 0)
    y_send(1)
    rows[pl.ds(0, rb), lanes(tp)] = picked[prow(tp), :]
    for a in range(3):
        wbuf[a, my_rows, lanes(tp)] = wsrc[a, frow(y * NX + 2 * px, 2), :]

    def run(event):
        kind, rest = event[0], event[1:]
        if kind == "T":
            ag_first(int(rest))
        elif kind == "A":
            ag_step(int(rest))
        elif kind == "R":
            y_relay("ab".index(rest))
        elif kind == "H":
            gate_up_here()
            hidden(0, nz - 1)
        else:
            q, g = int(rest[0]), "ab".index(rest[1])
            {"X": x_send, "F": x_forward, "C": core_send}[kind](q, g)

    for event in ORDER:
        if event == "H":
            with scope("scale0"):
                scale_of(0, 1)
        with scope(event):
            run(event)

    with scope("hid_last"):
        hidden(nz - 1, 1)

    rs_c = {}

    def rs_step(s, q):
        for d in (0, 1):
            if s == 0 and q not in SPLIT[d]:
                continue
            p = (up_of, down_of)[d](half - s)
            acc = part[at(p), chunk(q)]
            if (s - 1, d, q) in rs_c:
                rs_c[s - 1, d, q].wait_recv()
                acc = acc + rs_in[d, s - 1, q].astype(f32)
            rs_out[d, s, q] = acc.astype(bf16)
            rs_c[s, d, q] = send(
                rs_out.at[d, s, q],
                rs_in.at[d, s, q],
                rs_s.at[d, s, q],
                rs_r.at[d, s, q],
                z_dev[d],
            )

    for q in QORD:
        with scope(f"rs0_{q}"):
            d_c[q, 1].wait_recv()
            project(nz - 1, 1, q)
            rs_step(0, q)
    with scope("project"):
        for q in QORD:
            project(0, nz - 1, q)
        outs = []
        for a, out in enumerate((gate_out, up_out, down_out)):
            c = pltpu.make_async_copy(wbuf.at[a, frow(2 * core + h, 1), :], out, out_s.at[a])
            c.start()
            outs.append(c)
    for s in range(1, half):
        with scope(f"rs{s}"):
            for q in QORD:
                rs_step(s, q)

    fin = []
    mine = prow(tp)
    for q in QORD:
        with scope(f"last{q}"):
            acc = part[at(0), chunk(q)]
            for d in (0, 1):
                rs_c[half - 1, d, q].wait_recv()
                acc = acc + rs_in[d, half - 1, q].astype(f32)
            eo[:, chunk(q)] = acc.astype(bf16)
            for dx in range(NX):
                if q or dx:
                    t = plane(NX - q, dx)
                    fin.append(
                        send(
                            eo.at[:, lanes(t)],
                            ret.at[mine, :],
                            fin_s.at[q, dx],
                            fin_r.at[q, dx],
                            {"tp": t},
                        )
                    )
    ret[mine, :] = eo[:, lanes(tp)]
    with scope("fin"):
        ids = lax.broadcasted_iota(jnp.int32, (tr, NT * rb), 1).astype(f32)
        hots = [jnp.where(ids == cols8[:, k : k + 1], 1.0, 0.0).astype(bf16) for k in (0, 1)]
        for c in fin:
            c.wait_recv()
    with scope("mix"):
        sent = [jnp.dot(m, ret[...], preferred_element_type=f32) for m in hots]
        mixed_out[...] = (cols8[:, 2:3] * sent[0] + cols8[:, 3:4] * sent[1]).astype(bf16)
    with scope("drain"):
        for c in outs:
            c.wait()
        for c in pending:
            c.wait_send()


def exchange(tokens, gain, gate, up, down, routes, logits, nz):
    tr = tokens.shape[0]
    width, fb = NT * LANES, gate.shape[0] // NT
    rb = 2 * tr // NT
    half = nz // 2
    bf16, f32 = jnp.bfloat16, jnp.float32
    dma = pltpu.SemaphoreType.DMA
    hbm = pl.BlockSpec(memory_space=pl.ANY)
    served = jax.ShapeDtypeStruct((fb, width), bf16)
    return pl.pallas_call(
        functools.partial(kernel, nz),
        name="exchange",
        out_shape=[served, served, served, jax.ShapeDtypeStruct((tr, LANES), bf16)],
        in_specs=[hbm] * 7,
        out_specs=[hbm, hbm, hbm, pl.BlockSpec(memory_space=pltpu.VMEM)],
        scratch_shapes=[
            pltpu.VMEM((tr, LANES), bf16),
            pltpu.VMEM((1, LANES), f32),
            pltpu.VMEM((3, NT * fb, LANES), f32),
            pltpu.VMEM((2, tr), jnp.int32),
            pltpu.VMEM((2, tr), f32),
            pltpu.VMEM((3, NT * fb, LANES), bf16),
            pltpu.VMEM((NT * rb, LANES), bf16),
            pltpu.VMEM((tr, 8), f32),
            pltpu.VMEM((nz * rb, width), bf16),
            pltpu.VMEM((nz * rb, 1), f32),
            pltpu.VMEM((NX - 1, 3, 2 * fb, LANES), bf16),
            pltpu.VMEM((2, 3, 2 * fb, LANES), bf16),
            pltpu.VMEM((3, 4 * fb, width), bf16),
            pltpu.VMEM((2, nz * rb, 2 * fb), bf16),
            pltpu.VMEM((nz * rb, width), f32),
            pltpu.VMEM((2, half, NX, rb, QC), bf16),
            pltpu.VMEM((2, half, NX, rb, QC), bf16),
            pltpu.VMEM((rb, width), bf16),
            pltpu.VMEM((NT * rb, LANES), bf16),
            dma((7,)),
            dma((NX, NX)),
            dma((NX, NX)),
            dma((2, half, NX)),
            dma((2, half, NX)),
            dma((NX - 1, NG, 2)),
            dma((NX - 1, NG, 2)),
            dma((NG, 2)),
            dma((NG, 2)),
            dma((NX, NG, 3)),
            dma((NX, NG, 3)),
            dma((NX, NG)),
            dma((NX, NG)),
            dma((2, half, NX)),
            dma((2, half, NX)),
            dma((NX, NX)),
            dma((NX, NX)),
            dma((3,)),
        ],
        compiler_params=pltpu.CompilerParams(collective_id=0, has_side_effects=True),
    )(tokens, gain, gate, up, down, routes, logits)


def local(tokens, norm_gain, gate_master, up_master, down_master, routes, route_logits):
    flat = lambda m: m.reshape(-1, LANES)
    nz = lax.axis_size("fs") // 2
    gate_serve, up_serve, down_serve, mixed = exchange(
        tokens,
        norm_gain[None, :],
        flat(gate_master),
        flat(up_master),
        flat(down_master),
        routes.T,
        route_logits.T,
        nz,
    )
    return (gate_serve[None], up_serve[None], down_serve[None], mixed)


def solution(mesh):
    weights = P(None, "fs", "tp")
    served = P("tp", "fs", None)
    return jax.shard_map(
        local,
        mesh=mesh,
        in_specs=(P("fs", "tp"), P("tp"), weights, weights, weights, P("fs"), P("fs")),
        out_specs=(served, served, served, P("fs", "tp")),
        check_vma=False,
    )
```
